32 devices in a mesh: st: 8 (over z, x), tp: 4 (over y, core).
Axes of the slice: x: 2, y: 2, z: 4, core: 2. Of those that a mesh axis runs over, the one named last changes fastest.
Arguments:
- tokens: bfloat16 [4096, 2048], P('st'), may hold values from -6 to 6
- mix_query: bfloat16 [2048, 1024], P(None, 'tp'), may hold values from -0.125 to 0.125
- mix_key: bfloat16 [2048, 1024], P(None, 'tp'), may hold values from -0.125 to 0.125
- mix_value: bfloat16 [2048, 1024], P(None, 'tp'), may hold values from -0.125 to 0.125
- decay_lower_map: bfloat16 [2048, 64], replicated, may hold values from -0.125 to 0.125
- decay_upper_map: bfloat16 [64, 1024], P(None, 'tp'), may hold values from -1 to 1
- decay_base: float32 [1024], P('tp'), may hold values from -7.5 to -2.5
- decay_shift: float32 [4096, 16], P('st', 'tp'), may hold values from -3.8 to 9.8
- rate_lower_map: bfloat16 [2048, 64], replicated, may hold values from -0.125 to 0.125
- rate_upper_map: bfloat16 [64, 1024], P(None, 'tp'), may hold values from -0.75 to 0.75
- norm_gain: float32 [1024], P('tp'), may hold values from 0.1 to 1.9
- mix_out: bfloat16 [1024, 2048], P(None, 'tp'), may hold values from -0.1875 to 0.1875
- cross_query: bfloat16 [2048, 2048], P(None, 'tp'), may hold values from -0.125 to 0.125
- score_gain: float32 [2048], P('tp'), may hold values from 0.1 to 1.9
- passage_key: bfloat16 [2048, 2048], P(None, 'tp'), may hold values from -0.125 to 0.125
- passage_value: bfloat16 [2048, 2048], P(None, 'tp'), may hold values from -0.125 to 0.125
- cross_out: bfloat16 [2048, 2048], P(None, 'tp'), may hold values from -0.5 to 0.5
- gate_down: bfloat16 [2048, 128], replicated, may hold values from -0.125 to 0.125
- gate_up: bfloat16 [128, 2048], P(None, 'tp'), may hold values from -0.5 to 0.5
- store: bfloat16 [96, 96, 2048], P('st'), may hold values from -6 to 6
- passage_ids: int32 [64, 4], P('st'), may hold values from 0 to 95, as said below
Outputs:
- mixed: bfloat16 [4096, 2048], P('st', 'tp')
The draws below stay inside these ranges and needn't reach their ends.
Inputs may be any that keep to these rules, and one draw needn't show every extreme that they name: `passage_ids`: among the 32 passages named by the rows of one sequence, at most 4 are held by one index of st (passage p by index p // 12); in every draw exactly 4 are held by the index before the sequence's own.
All inputs are finite; a program needn't handle non-finite values.
Results may differ from the reference program's by a relative error of at most 0.0075.
Values may be sent and summed in bfloat16 or wider, within the bound.
A program may use at most 128 MiB of HBM per device.

```python
import jax
import jax.numpy as jnp
from jax import lax

MODEL_DIM = 2048
MIXER_HEADS = 16
RHEAD = 64
XHEADS = 8
XHEAD = 256
LOWRANK_WIDTH = 64
GLORA = 128
PLEN = 96
PER_BLOCK = 4
QBLOCK = 64
MBLOCK = 64
TOKENS_PER_SEQ = 512
PASS_DEV = 12
MIXER_WIDTH = 1024
XWIDTH = 2048
TOKEN_TOTAL = 4096
NPASS = 96
N_ST = 8


def draw_decay_shift(key, part):
    sequence_number = TOKEN_TOTAL // TOKENS_PER_SEQ
    span_count = TOKENS_PER_SEQ // MBLOCK
    base_key, spot_key, random_size_key = jax.random.split(key, 3)
    shift_baseline = jax.random.uniform(base_key, (sequence_number, span_count, 1, 1), jnp.float32, -0.8, 0.8)
    shift_baseline = jnp.broadcast_to(shift_baseline, (sequence_number, span_count, MBLOCK, MIXER_HEADS))
    shift_baseline = shift_baseline.reshape(sequence_number, TOKENS_PER_SEQ, MIXER_HEADS)
    spot_pos = jax.random.randint(spot_key, (sequence_number, 3, MIXER_HEADS), 0, TOKENS_PER_SEQ)
    target_location = jnp.arange(TOKENS_PER_SEQ)[None, :, None, None] == spot_pos[:, None, :, :]
    spike_addition = jnp.any(target_location, axis=2).astype(jnp.float32)
    spike_addition = spike_addition * jax.random.uniform(random_size_key, (sequence_number, TOKENS_PER_SEQ, MIXER_HEADS), jnp.float32, 7.0, 9.0)
    return (shift_baseline + spike_addition).reshape(TOKEN_TOTAL, MIXER_HEADS)


def draw_passage_ids(key, part):
    blk_dev = TOKENS_PER_SEQ // QBLOCK
    slot_count = blk_dev * PER_BLOCK
    capacity = max(2, -(-slot_count // N_ST))
    positions = N_ST * capacity

    def one_sequence(seq_key, seq_index):
        keys_five = jax.random.split(seq_key, 5)
        place = jnp.arange(positions)
        offset = place // capacity
        copy_idx = place % capacity
        forced = (offset == N_ST - 1) | (offset == N_ST // 2) & (copy_idx == 0)
        score = jax.random.randint(keys_five[0], (positions,), 0, 1 << 20)
        score = jnp.where(forced, -1, score) * positions + place
        chosen = jnp.argsort(score)[:slot_count]
        owner_of = (seq_index + offset[chosen]) % N_ST
        mixing = jax.random.randint(keys_five[1], (slot_count,), 0, 1 << 20) * slot_count + jnp.arange(slot_count)
        owner_of = owner_of[jnp.argsort(mixing)]
        local_idx = jax.random.randint(keys_five[2], (slot_count,), 0, PASS_DEV)
        local_idx = jnp.minimum(local_idx, jax.random.randint(keys_five[3], (slot_count,), 0, PASS_DEV))
        local_idx = jnp.minimum(local_idx, jax.random.randint(keys_five[4], (slot_count,), 0, PASS_DEV))
        return (owner_of * PASS_DEV + local_idx).reshape(blk_dev, PER_BLOCK)
    seq_keys = jax.random.split(jax.random.fold_in(key, 11), N_ST)
    picked = jax.vmap(one_sequence)(seq_keys, jnp.arange(N_ST))
    return picked.reshape(N_ST * blk_dev, PER_BLOCK).astype(jnp.int32)


def block_levels(own_key, shape, shards, least, high):
    factor_of = 1.0
    for dim, blocks in shards:
        heights = jax.random.uniform(jax.random.fold_in(jax.random.fold_in(own_key, 6), dim), (blocks,), jnp.float32, least / len(shards), high / len(shards))
        factor_of = factor_of * jnp.repeat(jnp.exp(heights), shape[dim] // blocks).reshape((-1,) + (1,) * (len(shape) - 1 - dim))
    return factor_of


def noise(own_key, shape, width, bound, cuts=(), dtype=jnp.bfloat16):
    level = block_levels(own_key, shape, cuts, -0.22, 0.18) if cuts else 1.0
    entries = jax.random.normal(own_key, shape, jnp.float32) * width * level
    return jnp.minimum(jnp.maximum(entries, -bound), bound).astype(dtype)


def setup_inputs(seed: int = 0) -> dict:
    keys = jax.random.split(jax.random.key(seed), 22)
    tokens = noise(keys[0], (TOKEN_TOTAL, MODEL_DIM), 1.0, 6.0, ((0, 8),))
    mix_query = noise(keys[1], (MODEL_DIM, MIXER_WIDTH), MODEL_DIM ** -0.5, 0.125, ((1, 4),))
    mix_key = noise(keys[2], (MODEL_DIM, MIXER_WIDTH), MODEL_DIM ** -0.5, 0.125, ((1, 4),))
    mix_value = noise(keys[3], (MODEL_DIM, MIXER_WIDTH), MODEL_DIM ** -0.5, 0.125, ((1, 4),))
    decay_lower_map = noise(keys[4], (MODEL_DIM, LOWRANK_WIDTH), MODEL_DIM ** -0.5, 0.125)
    decay_upper_map = noise(keys[5], (LOWRANK_WIDTH, MIXER_WIDTH), (LOWRANK_WIDTH // 2) ** -0.5, 1.0, ((1, 4),))
    decay_base = jnp.clip(-7.5 + 5.0 * jax.random.uniform(keys[6], (MIXER_WIDTH,), jnp.float32) ** block_levels(keys[6], (MIXER_WIDTH,), ((0, 4),), -0.2, 0.2), -7.5, -2.5)
    decay_shift = draw_decay_shift(jax.random.fold_in(keys[21], 71), 0)
    rate_lower_map = noise(keys[8], (MODEL_DIM, LOWRANK_WIDTH), MODEL_DIM ** -0.5, 0.125)
    rate_upper_map = noise(keys[9], (LOWRANK_WIDTH, MIXER_WIDTH), LOWRANK_WIDTH ** -0.5, 0.75, ((1, 4),))
    norm_gain = jnp.clip(1.0 + 0.18 * jax.random.normal(keys[10], (MIXER_WIDTH,), jnp.float32), 0.1, 1.9)
    mix_out = noise(keys[11], (MIXER_WIDTH, MODEL_DIM), MIXER_WIDTH ** -0.5, 0.1875, ((1, 4),))
    cross_query = noise(keys[12], (MODEL_DIM, XWIDTH), MODEL_DIM ** -0.5, 0.125, ((1, 4),))
    score_gain = jnp.clip(1.0 + 0.18 * jax.random.normal(keys[13], (XWIDTH,), jnp.float32), 0.1, 1.9)
    passage_key = noise(keys[14], (MODEL_DIM, XWIDTH), MODEL_DIM ** -0.5, 0.125, ((1, 4),))
    passage_value = noise(keys[15], (MODEL_DIM, XWIDTH), MODEL_DIM ** -0.5, 0.125, ((1, 4),))
    cross_out = noise(keys[16], (XWIDTH, MODEL_DIM), (XWIDTH // 16) ** -0.5, 0.5, ((1, 4),))
    gate_down = noise(keys[17], (MODEL_DIM, GLORA), MODEL_DIM ** -0.5, 0.125)
    gate_up = noise(keys[18], (GLORA, MODEL_DIM), GLORA ** -0.5, 0.5, ((1, 4),))
    store = noise(keys[19], (NPASS, PLEN, MODEL_DIM), 1.0, 6.0, ((0, 8),))
    passage_ids = draw_passage_ids(jax.random.fold_in(keys[21], 71), 0)
    return dict(tokens=tokens, mix_query=mix_query, mix_key=mix_key, mix_value=mix_value, decay_lower_map=decay_lower_map, decay_upper_map=decay_upper_map, decay_base=decay_base, decay_shift=decay_shift, rate_lower_map=rate_lower_map, rate_upper_map=rate_upper_map, norm_gain=norm_gain, mix_out=mix_out, cross_query=cross_query, score_gain=score_gain, passage_key=passage_key, passage_value=passage_value, cross_out=cross_out, gate_down=gate_down, gate_up=gate_up, store=store, passage_ids=passage_ids)


FLOAT32 = jnp.float32
BFLOAT = jnp.bfloat16
PRECISE = lax.Precision.HIGHEST

def rounded(values):
    return lax.optimization_barrier(values.astype(BFLOAT)).astype(FLOAT32)

def head_norm(values, head_size):
    shaped = values.reshape(values.shape[:-1] + (values.shape[-1] // head_size, head_size))
    scaled = shaped * lax.rsqrt(lax.optimization_barrier(jnp.mean(shaped * shaped, axis=-1, keepdims=True)) + 1e-06)
    return scaled.reshape(values.shape)

def recurrent_step(state, inputs):
    query_vec, fade_t, key_vec, value_vec, unit_key, rate_gate = inputs
    pulled = jnp.einsum('bhij,bhj->bhi', state, -unit_key, precision=PRECISE)
    state = state * fade_t[:, :, None, :] + pulled[..., :, None] * (unit_key * rate_gate)[..., None, :] + value_vec[..., :, None] * key_vec[..., None, :]
    return (state, jnp.einsum('bhij,bhj->bhi', state, query_vec, precision=PRECISE))

def reference(tokens, mix_query, mix_key, mix_value, decay_lower_map, decay_upper_map, decay_base, decay_shift, rate_lower_map, rate_upper_map, norm_gain, mix_out, cross_query, score_gain, passage_key, passage_value, cross_out, gate_down, gate_up, store, passage_ids):
    total_rows = tokens.shape[0]
    sequence_number = total_rows // TOKENS_PER_SEQ

    def project(weight):
        return rounded(jnp.dot(tokens, weight, preferred_element_type=FLOAT32))
    query_vec = project(mix_query)
    key_vec = project(mix_key)
    value_vec = project(mix_value)
    decay_low = jnp.tanh(jnp.dot(tokens, decay_lower_map, preferred_element_type=FLOAT32)).astype(BFLOAT)
    decay_pre = decay_base + jnp.dot(decay_low, decay_upper_map, preferred_element_type=FLOAT32) + jnp.repeat(decay_shift, RHEAD, axis=1)
    log_fade = -jnp.exp(-jax.nn.softplus(-decay_pre) - 0.5)
    rate_low = jnp.dot(tokens, rate_lower_map, preferred_element_type=FLOAT32).astype(BFLOAT)
    rate_gate = jax.nn.sigmoid(jnp.dot(rate_low, rate_upper_map, preferred_element_type=FLOAT32))

    def by_time(values):
        return jnp.moveaxis(values.reshape(sequence_number, TOKENS_PER_SEQ, MIXER_HEADS, RHEAD), 1, 0)
    keyed = key_vec.reshape(total_rows, MIXER_HEADS, RHEAD)
    unit_key = keyed * lax.rsqrt(lax.optimization_barrier(jnp.sum(keyed * keyed, axis=-1, keepdims=True)) + 1e-06)
    sequence_in = (by_time(query_vec), by_time(jnp.exp(log_fade)), by_time(key_vec), by_time(value_vec), by_time(unit_key), by_time(rate_gate))
    state_zero = jnp.zeros((sequence_number, MIXER_HEADS, RHEAD, RHEAD), FLOAT32)
    _, head_out = lax.scan(recurrent_step, state_zero, sequence_in)
    head_out = jnp.moveaxis(head_out, 0, 1).reshape(total_rows, MIXER_HEADS, RHEAD)
    centred = head_out - lax.optimization_barrier(jnp.mean(head_out, axis=-1, keepdims=True))
    spread = lax.optimization_barrier(jnp.mean(centred * centred, axis=-1, keepdims=True))
    mixer_heads = (centred * lax.rsqrt(spread + 0.00064)).reshape(total_rows, MIXER_WIDTH)
    mixer_heads = (mixer_heads * norm_gain).astype(BFLOAT)
    queries = head_norm(jnp.dot(tokens, cross_query, preferred_element_type=FLOAT32), XHEAD) * score_gain
    queries = queries.astype(BFLOAT)
    store_rows = store.reshape(-1, MODEL_DIM)
    keys_all = head_norm(jnp.dot(store_rows, passage_key, preferred_element_type=FLOAT32), XHEAD)
    keys_all = keys_all.astype(BFLOAT).reshape(-1, PLEN, XWIDTH)
    values_all = jnp.dot(store_rows, passage_value, preferred_element_type=FLOAT32).astype(BFLOAT)
    values_all = values_all.reshape(-1, PLEN, XWIDTH)

    def attend(item):
        block_q, block_ids = item
        block_keys = keys_all[block_ids].reshape(-1, XHEADS, XHEAD).astype(FLOAT32)
        block_values = values_all[block_ids].reshape(-1, XHEADS, XHEAD).astype(FLOAT32)
        block_q = block_q.reshape(QBLOCK, XHEADS, XHEAD).astype(FLOAT32)
        scores = jnp.einsum('qhd,khd->hqk', block_q, block_keys, precision=PRECISE) * XHEAD ** (-0.5)
        expon = jnp.exp(scores)
        weights = rounded(expon / lax.optimization_barrier(jnp.sum(expon, axis=-1, keepdims=True)))
        result = jnp.einsum('hqk,khd->qhd', weights, block_values, precision=PRECISE)
        return result.astype(BFLOAT).reshape(QBLOCK, XWIDTH)
    attended = lax.map(attend, (queries.reshape(-1, QBLOCK, XWIDTH), passage_ids)).reshape(total_rows, XWIDTH)
    gate_low = jnp.dot(tokens, gate_down, preferred_element_type=FLOAT32).astype(BFLOAT)
    gate_open = jax.nn.sigmoid(jnp.dot(gate_low, gate_up, preferred_element_type=FLOAT32))
    mixer_part = jnp.dot(mixer_heads, mix_out, preferred_element_type=FLOAT32)
    cross_part = jnp.dot(attended, cross_out, preferred_element_type=FLOAT32)
    return (mixer_part + gate_open * cross_part).astype(BFLOAT)
```

```python
import functools

import jax
import jax.numpy as jnp
from jax import lax
from jax.experimental import pallas as pl
from jax.experimental.pallas import tpu as pltpu
from jax.sharding import PartitionSpec as P


XHEAD = 256
QBLOCK = 64
MBLOCK = 64


FLOAT32 = jnp.float32
BFLOAT = jnp.bfloat16


def head_norm(values, head_size):
    shaped = values.reshape(values.shape[:-1] + (values.shape[-1] // head_size, head_size))
    scaled = shaped * lax.rsqrt(jnp.mean(shaped * shaped, axis=-1, keepdims=True) + 1e-06)
    return scaled.reshape(values.shape)


def split(values):
    high = values.astype(BFLOAT)
    return high, (values - high.astype(FLOAT32)).astype(BFLOAT)


def raw_dot(left, right, dims):
    return lax.dot_general(left, right, (dims, ((), ())), preferred_element_type=FLOAT32)


def fine_dot(left, right, dims=((1,), (0,))):
    left_high, left_low = left if isinstance(left, tuple) else split(left)
    right_high, right_low = right if isinstance(right, tuple) else split(right)
    return raw_dot(left_high, right_high, dims) + (
        raw_dot(left_high, right_low, dims) + raw_dot(left_low, right_high, dims)
    )


def exact_dot(values, ones):
    high, low = split(values)
    return raw_dot(high, ones, ((1,), (0,))) + raw_dot(low, ones, ((1,), (0,)))


def mixer_kernel(
    heads, blocks, query_ref, key_ref, value_ref, fade_ref, gate_ref, gain_ref, out_ref, state_ref
):
    width = query_ref.shape[1]
    size = width // heads
    rows = heads * MBLOCK

    @pl.when(pl.program_id(0) == 0)
    def _():
        state_ref[...] = jnp.zeros_like(state_ref)

    def iota(shape, dim):
        return lax.broadcasted_iota(jnp.int32, shape, dim)

    row_head = (iota((rows, width), 0) // MBLOCK) == (iota((rows, width), 1) // size)
    state_head = (iota((width, width), 0) // size) == (iota((width, width), 1) // size)
    ones_head = jnp.where(state_head, 1.0, 0.0).astype(BFLOAT)
    row_pos = iota((rows, rows), 0) % MBLOCK
    col_pos = iota((rows, rows), 1) % MBLOCK
    strict = col_pos < row_pos
    upto = col_pos <= row_pos
    lower = jnp.where(
        iota((MBLOCK, MBLOCK), 1) <= iota((MBLOCK, MBLOCK), 0), 1.0, 0.0
    ).astype(BFLOAT)

    def expand(values):
        return jnp.where(row_head, jnp.concatenate([values] * heads, axis=0), 0.0)

    def compact(values):
        return jnp.concatenate(
            [values[:, head * size : (head + 1) * size] for head in range(heads)], axis=0
        )

    def natural(values):
        return jnp.concatenate(
            [values[head * MBLOCK : (head + 1) * MBLOCK] for head in range(heads)], axis=1
        )

    def each(fn, *lists):
        return [fn(*items) for items in zip(*lists)]

    def load(ref):
        return [ref[pl.ds(b * MBLOCK, MBLOCK), :].astype(FLOAT32) for b in range(blocks)]

    def running_sum(fade):
        high, low = split(fade)
        rest = (fade - high.astype(FLOAT32) - low.astype(FLOAT32)).astype(BFLOAT)
        dims = ((1,), (0,))
        return raw_dot(lower, high, dims) + (raw_dot(lower, low, dims) + raw_dot(lower, rest, dims))

    query, key, value = load(query_ref), load(key_ref), load(value_ref)
    fade, gate = load(fade_ref), load(gate_ref)
    cumul = each(running_sum, fade)
    unit = each(lambda k: k * lax.rsqrt(exact_dot(k * k, ones_head) + 1e-06), key)
    rate = each(lambda u, g: u * g, unit, gate)
    minus_scaled = each(lambda u, c, f: -u * jnp.exp(c - f), unit, cumul, fade)
    query_scaled = each(lambda q, c: q * jnp.exp(c), query, cumul)
    inverse = each(lambda c: jnp.exp(-c), cumul)
    fade_out = each(lambda c: jnp.exp(c[MBLOCK - 1 :, :] - c), cumul)
    block_fade = each(lambda c: jnp.exp(c[MBLOCK - 1 :, :]), cumul)
    left = each(
        lambda m, q: split(jnp.concatenate([expand(m), expand(q)], axis=0)),
        minus_scaled,
        query_scaled,
    )
    right = each(
        lambda k, r, i: split(jnp.concatenate([expand(k * i), expand(r * i)], axis=0)),
        key,
        rate,
        inverse,
    )
    pairs = each(lambda a, b: fine_dot(a, b, ((1,), (1,))), left, right)
    key_mats = each(
        lambda p: jnp.concatenate(
            [jnp.where(strict, p[:rows, :rows], 0.0), jnp.where(upto, p[rows:, :rows], 0.0)], axis=0
        ),
        pairs,
    )
    rate_pull = each(lambda p: split(jnp.where(strict, p[:rows, rows:], 0.0)), pairs)
    rate_read = each(lambda p: split(jnp.where(upto, p[rows:, rows:], 0.0)), pairs)
    value_rows = each(lambda v: compact(v).astype(BFLOAT), value)

    def key_values(mats, vals):
        high, low = split(mats)
        return raw_dot(high, vals, ((1,), (0,))) + raw_dot(low, vals, ((1,), (0,)))

    from_values = each(key_values, key_mats, value_rows)
    solved = each(
        lambda m, kv: jnp.concatenate([compact(m), kv[:rows]], axis=1), minus_scaled, from_values
    )
    power = rate_pull
    levels = (MBLOCK - 1).bit_length()
    for level in range(levels):
        solved = each(lambda s, p: s + fine_dot(p, s), solved, power)
        if level < levels - 1:
            power = each(lambda p: split(fine_dot(p, p)), power)
    solved_halves = each(split, solved)
    reads = each(
        lambda q, kv, r, s: jnp.concatenate([compact(q), kv[rows:]], axis=1) + fine_dot(r, s),
        query_scaled,
        from_values,
        rate_read,
        solved_halves,
    )
    moved = each(
        lambda s, r, f: fine_dot(s, expand(r * f), ((0,), (0,))), solved_halves, rate, fade_out
    )

    def key_update(vals, k, f):
        high, low = split(expand(k * f))
        dims = ((0,), (0,))
        return raw_dot(vals, high, dims) + raw_dot(vals, low, dims)

    added = each(key_update, value_rows, key, fade_out)
    carry = each(
        lambda m: split(jnp.where(state_head, jnp.concatenate([m[:size]] * heads, axis=0), 0.0)),
        moved,
    )
    added = each(lambda a, m: a + m[size:], added, moved)
    read_state = each(lambda r: split(natural(r[:, :size])), reads)
    read_fixed = each(lambda r: natural(r[:, size:]), reads)
    state = state_ref[...]
    head_out = []
    for block in range(blocks):
        spread_state = jnp.where(state_head, jnp.concatenate([state] * heads, axis=0), 0.0)
        head_out.append(
            read_fixed[block] + fine_dot(read_state[block], spread_state, ((1,), (1,)))
        )
        state = state * block_fade[block] + fine_dot(state, carry[block]) + added[block]
    state_ref[...] = state
    for block in range(blocks):
        mean = exact_dot(head_out[block], ones_head) * (1.0 / size)
        centred = head_out[block] - mean
        variance = exact_dot(centred * centred, ones_head) * (1.0 / size)
        normed = centred * lax.rsqrt(variance + 0.00064) * gain_ref[...]
        out_ref[pl.ds(block * MBLOCK, MBLOCK), :] = normed.astype(BFLOAT)


def recurrence(heads, query_vec, key_vec, value_vec, log_fade, rate_gate, norm_gain):
    rows, width = query_vec.shape
    blocks = 2 if rows % (2 * MBLOCK) == 0 else 1
    step = blocks * MBLOCK
    piece = pl.BlockSpec((step, width), lambda i: (i, 0))
    return pl.pallas_call(
        functools.partial(mixer_kernel, heads, blocks),
        grid=(rows // step,),
        in_specs=[piece] * 5 + [pl.BlockSpec((1, width), lambda i: (0, 0))],
        out_specs=piece,
        out_shape=jax.ShapeDtypeStruct((rows, width), BFLOAT),
        scratch_shapes=[pltpu.VMEM((width // heads, width), FLOAT32)],
        compiler_params=pltpu.CompilerParams(
            dimension_semantics=("arbitrary",), vmem_limit_bytes=48 * 1024 * 1024
        ),
        cost_estimate=pl.CostEstimate(
            flops=rows * width * 40000, bytes_accessed=rows * width * 16, transcendentals=0
        ),
    )(query_vec, key_vec, value_vec, log_fade, rate_gate, norm_gain.reshape(1, width))


def partial_kernel(heads, per_step, ids_ref, query_ref, key_ref, value_ref, out_ref, sum_ref):
    base = pl.program_id(0) * per_step
    length = key_ref.shape[1]
    ones = jnp.ones((8, length), BFLOAT)
    for slot in range(per_step):
        passage = ids_ref[base + slot]
        for head in range(heads):
            span = pl.ds(head * XHEAD, XHEAD)
            scores = raw_dot(
                query_ref[slot, :, span], key_ref[passage, :, span], ((1,), (1,))
            ) * XHEAD ** (-0.5)
            expon = jnp.exp(scores).astype(BFLOAT)
            out_ref[slot, :, span] = raw_dot(
                expon, value_ref[passage, :, span], ((1,), (0,))
            ).astype(BFLOAT)
            sums = raw_dot(ones, expon, ((1,), (1,)))
            sum_ref[slot, pl.ds(head, 1), :] = sums[:1]


def partial_attention(ids, queries, keys, values):
    slots, tokens, width = queries.shape
    heads = width // XHEAD
    per_step = 4 if slots % 4 == 0 else 2
    whole = pl.BlockSpec(keys.shape, lambda i, ids: (0, 0, 0))
    return pl.pallas_call(
        functools.partial(partial_kernel, heads, per_step),
        grid_spec=pltpu.PrefetchScalarGridSpec(
            num_scalar_prefetch=1,
            grid=(slots // per_step,),
            in_specs=[
                pl.BlockSpec((per_step, tokens, width), lambda i, ids: (i, 0, 0)),
                whole,
                whole,
            ],
            out_specs=[
                pl.BlockSpec((per_step, tokens, width), lambda i, ids: (i, 0, 0)),
                pl.BlockSpec((per_step, heads, tokens), lambda i, ids: (i, 0, 0)),
            ],
        ),
        out_shape=[
            jax.ShapeDtypeStruct((slots, tokens, width), BFLOAT),
            jax.ShapeDtypeStruct((slots, heads, tokens), FLOAT32),
        ],
        compiler_params=pltpu.CompilerParams(
            dimension_semantics=("arbitrary",), vmem_limit_bytes=32 * 1024 * 1024
        ),
        cost_estimate=pl.CostEstimate(
            flops=slots * tokens * width * keys.shape[1] * 4,
            bytes_accessed=slots * tokens * width * 4,
            transcendentals=0,
        ),
    )(ids, queries, keys, values)


def combine_kernel(heads, where_ref, *refs):
    *part_refs, scale_ref, out_ref = refs
    for head in range(heads):
        span = pl.ds(head * XHEAD, XHEAD)
        total = part_refs[0][0, :, span].astype(FLOAT32)
        for part in part_refs[1:]:
            total = total + part[0, :, span].astype(FLOAT32)
        out_ref[:, span] = (total * scale_ref[0, :, head : head + 1]).astype(BFLOAT)


def combine(where, parts, scale):
    blocks, per_block = where.shape
    _, tokens, width = parts.shape
    heads = width // XHEAD

    def part_spec(place):
        return pl.BlockSpec(
            (1, tokens, width), lambda i, where: (where[i * per_block + place], 0, 0)
        )

    return pl.pallas_call(
        functools.partial(combine_kernel, heads),
        grid_spec=pltpu.PrefetchScalarGridSpec(
            num_scalar_prefetch=1,
            grid=(blocks,),
            in_specs=[part_spec(place) for place in range(per_block)]
            + [pl.BlockSpec((1, tokens, heads), lambda i, where: (i, 0, 0))],
            out_specs=pl.BlockSpec((tokens, width), lambda i, where: (i, 0)),
        ),
        out_shape=jax.ShapeDtypeStruct((blocks * tokens, width), BFLOAT),
        compiler_params=pltpu.CompilerParams(dimension_semantics=("arbitrary",)),
    )(where.reshape(-1), *([parts] * per_block), scale)


def mixer(
    tokens,
    mix_query,
    mix_key,
    mix_value,
    decay_lower_map,
    decay_upper_map,
    decay_base,
    decay_shift,
    rate_lower_map,
    rate_upper_map,
    norm_gain,
):
    head_count = decay_shift.shape[1]
    head_size = mix_query.shape[1] // head_count

    def project(weight):
        return jnp.dot(tokens, weight, preferred_element_type=FLOAT32).astype(BFLOAT)

    query_vec = project(mix_query)
    key_vec = project(mix_key)
    value_vec = project(mix_value)
    decay_low = jnp.tanh(
        jnp.dot(tokens, decay_lower_map, preferred_element_type=FLOAT32)
    ).astype(BFLOAT)
    decay_pre = (
        decay_base
        + jnp.dot(decay_low, decay_upper_map, preferred_element_type=FLOAT32)
        + jnp.repeat(decay_shift, head_size, axis=1)
    )
    log_fade = -jnp.exp(-jax.nn.softplus(-decay_pre) - 0.5)
    rate_low = jnp.dot(tokens, rate_lower_map, preferred_element_type=FLOAT32).astype(BFLOAT)
    rate_gate = jax.nn.sigmoid(jnp.dot(rate_low, rate_upper_map, preferred_element_type=FLOAT32))
    return recurrence(
        head_count, query_vec, key_vec, value_vec, log_fade, rate_gate, norm_gain
    )


def layer(
    tokens,
    mix_query,
    mix_key,
    mix_value,
    decay_lower_map,
    decay_upper_map,
    decay_base,
    decay_shift,
    rate_lower_map,
    rate_upper_map,
    norm_gain,
    mix_out,
    cross_query,
    score_gain,
    passage_key,
    passage_value,
    cross_out,
    gate_down,
    gate_up,
    store,
    passage_ids,
):
    model_width = tokens.shape[1]
    owner_count = lax.axis_size("st")
    pass_dev = store.shape[0]
    passage_len = store.shape[1]
    cross_width = cross_query.shape[1]
    head_count = cross_width // XHEAD
    block_count, per_block = passage_ids.shape
    flat_ids = passage_ids.reshape(-1)
    slot_count = flat_ids.shape[0]
    capacity = max(2, -(-slot_count // owner_count))
    owner_of = flat_ids // pass_dev
    local_idx = flat_ids % pass_dev
    slot_order = jnp.arange(slot_count)
    earlier_same = (owner_of[:, None] == owner_of[None, :]) & (
        slot_order[None, :] < slot_order[:, None]
    )
    slot_rank = jnp.sum(earlier_same.astype(jnp.int32), axis=1)
    to_owner = owner_of[:, None] == jnp.arange(owner_count)[None, :]
    to_slot = slot_rank[:, None] == jnp.arange(capacity)[None, :]
    chosen = to_owner[:, :, None] & to_slot[:, None, :]
    wanted = jnp.sum(jnp.where(chosen, local_idx[:, None, None], 0), axis=0)
    asking = jnp.sum(jnp.where(chosen, (slot_order // per_block)[:, None, None], 0), axis=0)
    where_from = owner_of * capacity + slot_rank

    served = lax.all_to_all(wanted, "st", split_axis=0, concat_axis=0, tiled=True).reshape(-1)
    queries = (
        head_norm(jnp.dot(tokens, cross_query, preferred_element_type=FLOAT32), XHEAD)
        * score_gain
    )
    queries = queries.astype(BFLOAT).reshape(block_count, QBLOCK, cross_width)
    outgoing = queries[asking.reshape(-1)].reshape(
        owner_count, capacity, QBLOCK, cross_width
    )
    incoming = lax.all_to_all(outgoing, "st", split_axis=0, concat_axis=0, tiled=True)
    flat_rows = store.reshape(-1, model_width)
    keyed = head_norm(
        jnp.dot(flat_rows, passage_key, preferred_element_type=FLOAT32), XHEAD
    ).astype(BFLOAT)
    valued = jnp.dot(flat_rows, passage_value, preferred_element_type=FLOAT32).astype(BFLOAT)
    keyed = keyed.reshape(pass_dev, passage_len, cross_width)
    valued = valued.reshape(pass_dev, passage_len, cross_width)
    parts, sums = partial_attention(
        served,
        incoming.reshape(owner_count * capacity, QBLOCK, cross_width),
        keyed,
        valued,
    )
    sums = lax.all_to_all(
        sums.reshape(owner_count, capacity, head_count, QBLOCK),
        "st",
        split_axis=0,
        concat_axis=0,
        tiled=True,
    )
    parts = lax.all_to_all(
        parts.reshape(owner_count, capacity, QBLOCK, cross_width),
        "st",
        split_axis=0,
        concat_axis=0,
        tiled=True,
    )
    mixer_heads = mixer(
        tokens,
        mix_query,
        mix_key,
        mix_value,
        decay_lower_map,
        decay_upper_map,
        decay_base,
        decay_shift,
        rate_lower_map,
        rate_upper_map,
        norm_gain,
    )
    sums = sums.reshape(owner_count * capacity, head_count, QBLOCK)[where_from]
    sums = jnp.sum(sums.reshape(block_count, per_block, head_count, QBLOCK), axis=1)
    scale = (1.0 / sums).transpose(0, 2, 1)
    attended = combine(
        where_from.reshape(block_count, per_block),
        parts.reshape(owner_count * capacity, QBLOCK, cross_width),
        scale,
    )
    shard_total = lax.axis_size("tp")
    out_cols = mix_out.shape[1]
    mix_rows = mix_out.reshape(shard_total, -1, out_cols)
    cross_rows = cross_out.reshape(shard_total, -1, out_cols)
    mixer_part = jnp.einsum(
        "ntc,ncd->td",
        lax.all_gather(mixer_heads[None], "tp", axis=0, tiled=True),
        mix_rows,
        preferred_element_type=FLOAT32,
    )
    gate_low = jnp.dot(tokens, gate_down, preferred_element_type=FLOAT32).astype(BFLOAT)
    gate_open = jax.nn.sigmoid(jnp.dot(gate_low, gate_up, preferred_element_type=FLOAT32))
    cross_part = jnp.einsum(
        "ntc,ncd->td",
        lax.all_gather(attended[None], "tp", axis=0, tiled=True),
        cross_rows,
        preferred_element_type=FLOAT32,
    )
    return (mixer_part + gate_open * cross_part).astype(BFLOAT)


def solution(mesh):
    placed = (
        P("st", None),
        P(None, "tp"),
        P(None, "tp"),
        P(None, "tp"),
        P(),
        P(None, "tp"),
        P("tp"),
        P("st", "tp"),
        P(),
        P(None, "tp"),
        P("tp"),
        P(None, "tp"),
        P(None, "tp"),
        P("tp"),
        P(None, "tp"),
        P(None, "tp"),
        P(None, "tp"),
        P(),
        P(None, "tp"),
        P("st", None, None),
        P("st", None),
    )
    return jax.shard_map(
        layer, mesh=mesh, in_specs=placed, out_specs=P("st", "tp"), check_vma=False
    )
```

```python
import functools

import jax
import jax.numpy as jnp
from jax import lax
from jax.experimental import pallas as pl
from jax.experimental.pallas import tpu as pltpu
from jax.sharding import PartitionSpec as P


XHEAD = 256
QBLOCK = 64
MBLOCK = 64


FLOAT32 = jnp.float32
BFLOAT = jnp.bfloat16


def head_norm(values, head_size):
    shaped = values.reshape(values.shape[:-1] + (values.shape[-1] // head_size, head_size))
    scaled = shaped * lax.rsqrt(jnp.mean(shaped * shaped, axis=-1, keepdims=True) + 1e-06)
    return scaled.reshape(values.shape)


def split(values):
    high = values.astype(BFLOAT)
    return high, (values - high.astype(FLOAT32)).astype(BFLOAT)


def raw_dot(left, right, dims):
    return lax.dot_general(left, right, (dims, ((), ())), preferred_element_type=FLOAT32)


def fine_dot(left, right, dims=((1,), (0,))):
    left_high, left_low = left if isinstance(left, tuple) else split(left)
    right_high, right_low = right if isinstance(right, tuple) else split(right)
    return raw_dot(left_high, right_high, dims) + (
        raw_dot(left_high, right_low, dims) + raw_dot(left_low, right_high, dims)
    )


def exact_dot(values, ones):
    high, low = split(values)
    return raw_dot(high, ones, ((1,), (0,))) + raw_dot(low, ones, ((1,), (0,)))


def mixer_kernel(
    heads, blocks, query_ref, key_ref, value_ref, fade_ref, gate_ref, gain_ref, out_ref, state_ref
):
    width = query_ref.shape[1]
    size = width // heads
    rows = heads * MBLOCK

    @pl.when(pl.program_id(0) == 0)
    def _():
        state_ref[...] = jnp.zeros_like(state_ref)

    def iota(shape, dim):
        return lax.broadcasted_iota(jnp.int32, shape, dim)

    row_head = (iota((rows, width), 0) // MBLOCK) == (iota((rows, width), 1) // size)
    state_head = (iota((width, width), 0) // size) == (iota((width, width), 1) // size)
    ones_head = jnp.where(state_head, 1.0, 0.0).astype(BFLOAT)
    row_pos = iota((rows, rows), 0) % MBLOCK
    col_pos = iota((rows, rows), 1) % MBLOCK
    strict = col_pos < row_pos
    upto = col_pos <= row_pos
    lower = jnp.where(
        iota((MBLOCK, MBLOCK), 1) <= iota((MBLOCK, MBLOCK), 0), 1.0, 0.0
    ).astype(BFLOAT)

    def expand(values):
        return jnp.where(row_head, jnp.concatenate([values] * heads, axis=0), 0.0)

    def compact(values):
        return jnp.concatenate(
            [values[:, head * size : (head + 1) * size] for head in range(heads)], axis=0
        )

    def natural(values):
        return jnp.concatenate(
            [values[head * MBLOCK : (head + 1) * MBLOCK] for head in range(heads)], axis=1
        )

    def each(fn, *lists):
        return [fn(*items) for items in zip(*lists)]

    def load(ref):
        return [ref[pl.ds(b * MBLOCK, MBLOCK), :].astype(FLOAT32) for b in range(blocks)]

    def running_sum(fade):
        high, low = split(fade)
        rest = (fade - high.astype(FLOAT32) - low.astype(FLOAT32)).astype(BFLOAT)
        dims = ((1,), (0,))
        return raw_dot(lower, high, dims) + (raw_dot(lower, low, dims) + raw_dot(lower, rest, dims))

    query, key, value = load(query_ref), load(key_ref), load(value_ref)
    fade, gate = load(fade_ref), load(gate_ref)
    cumul = each(running_sum, fade)
    unit = each(lambda k: k * lax.rsqrt(exact_dot(k * k, ones_head) + 1e-06), key)
    rate = each(lambda u, g: u * g, unit, gate)
    minus_scaled = each(lambda u, c, f: -u * jnp.exp(c - f), unit, cumul, fade)
    query_scaled = each(lambda q, c: q * jnp.exp(c), query, cumul)
    inverse = each(lambda c: jnp.exp(-c), cumul)
    fade_out = each(lambda c: jnp.exp(c[MBLOCK - 1 :, :] - c), cumul)
    block_fade = each(lambda c: jnp.exp(c[MBLOCK - 1 :, :]), cumul)
    left = each(
        lambda m, q: split(jnp.concatenate([expand(m), expand(q)], axis=0)),
        minus_scaled,
        query_scaled,
    )
    right = each(
        lambda k, r, i: split(jnp.concatenate([expand(k * i), expand(r * i)], axis=0)),
        key,
        rate,
        inverse,
    )
    pairs = each(lambda a, b: fine_dot(a, b, ((1,), (1,))), left, right)
    key_mats = each(
        lambda p: jnp.concatenate(
            [jnp.where(strict, p[:rows, :rows], 0.0), jnp.where(upto, p[rows:, :rows], 0.0)], axis=0
        ),
        pairs,
    )
    rate_pull = each(lambda p: split(jnp.where(strict, p[:rows, rows:], 0.0)), pairs)
    rate_read = each(lambda p: split(jnp.where(upto, p[rows:, rows:], 0.0)), pairs)
    value_rows = each(lambda v: compact(v).astype(BFLOAT), value)

    def key_values(mats, vals):
        high, low = split(mats)
        return raw_dot(high, vals, ((1,), (0,))) + raw_dot(low, vals, ((1,), (0,)))

    from_values = each(key_values, key_mats, value_rows)
    solved = each(
        lambda m, kv: jnp.concatenate([compact(m), kv[:rows]], axis=1), minus_scaled, from_values
    )
    power = rate_pull
    levels = (MBLOCK - 1).bit_length()
    for level in range(levels):
        solved = each(lambda s, p: s + fine_dot(p, s), solved, power)
        if level < levels - 1:
            power = each(lambda p: split(fine_dot(p, p)), power)
    solved_halves = each(split, solved)
    reads = each(
        lambda q, kv, r, s: jnp.concatenate([compact(q), kv[rows:]], axis=1) + fine_dot(r, s),
        query_scaled,
        from_values,
        rate_read,
        solved_halves,
    )
    moved = each(
        lambda s, r, f: fine_dot(s, expand(r * f), ((0,), (0,))), solved_halves, rate, fade_out
    )

    def key_update(vals, k, f):
        high, low = split(expand(k * f))
        dims = ((0,), (0,))
        return raw_dot(vals, high, dims) + raw_dot(vals, low, dims)

    added = each(key_update, value_rows, key, fade_out)
    carry = each(
        lambda m: split(jnp.where(state_head, jnp.concatenate([m[:size]] * heads, axis=0), 0.0)),
        moved,
    )
    added = each(lambda a, m: a + m[size:], added, moved)
    read_state = each(lambda r: split(natural(r[:, :size])), reads)
    read_fixed = each(lambda r: natural(r[:, size:]), reads)
    state = state_ref[...]
    head_out = []
    for block in range(blocks):
        spread_state = jnp.where(state_head, jnp.concatenate([state] * heads, axis=0), 0.0)
        head_out.append(
            read_fixed[block] + fine_dot(read_state[block], spread_state, ((1,), (1,)))
        )
        state = state * block_fade[block] + fine_dot(state, carry[block]) + added[block]
    state_ref[...] = state
    for block in range(blocks):
        mean = exact_dot(head_out[block], ones_head) * (1.0 / size)
        centred = head_out[block] - mean
        variance = exact_dot(centred * centred, ones_head) * (1.0 / size)
        normed = centred * lax.rsqrt(variance + 0.00064) * gain_ref[...]
        out_ref[pl.ds(block * MBLOCK, MBLOCK), :] = normed.astype(BFLOAT)


def recurrence(heads, query_vec, key_vec, value_vec, log_fade, rate_gate, norm_gain):
    rows, width = query_vec.shape
    blocks = 2 if rows % (2 * MBLOCK) == 0 else 1
    step = blocks * MBLOCK
    piece = pl.BlockSpec((step, width), lambda i: (i, 0))
    return pl.pallas_call(
        functools.partial(mixer_kernel, heads, blocks),
        grid=(rows // step,),
        in_specs=[piece] * 5 + [pl.BlockSpec((1, width), lambda i: (0, 0))],
        out_specs=piece,
        out_shape=jax.ShapeDtypeStruct((rows, width), BFLOAT),
        scratch_shapes=[pltpu.VMEM((width // heads, width), FLOAT32)],
        compiler_params=pltpu.CompilerParams(
            dimension_semantics=("arbitrary",), vmem_limit_bytes=48 * 1024 * 1024
        ),
        cost_estimate=pl.CostEstimate(
            flops=rows * width * 40000, bytes_accessed=rows * width * 16, transcendentals=0
        ),
    )(query_vec, key_vec, value_vec, log_fade, rate_gate, norm_gain.reshape(1, width))


def pack_kernel(capacity, asking_ref, wanted_ref, dots_ref, gain_ref, *refs):
    *out_refs, held = refs
    owner = pl.program_id(0)
    heads = len(out_refs)

    @pl.when(owner == 0)
    def _():
        for head in range(heads):
            span = pl.ds(head * XHEAD, XHEAD)
            for block in range(held.shape[0]):
                dots = dots_ref[pl.ds(block * QBLOCK, QBLOCK), span]
                mean = jnp.mean(dots * dots, axis=-1, keepdims=True)
                held[block, :, span] = (
                    dots * lax.rsqrt(mean + 1e-06) * gain_ref[:, span]
                ).astype(BFLOAT)

    extra = out_refs[0].shape[1] - capacity * QBLOCK
    row = lax.broadcasted_iota(jnp.int32, (extra, XHEAD), 0)
    names = jnp.zeros((extra, XHEAD), FLOAT32)
    for slot in range(capacity):
        block = asking_ref[owner * capacity + slot]
        names = jnp.where(row == slot, wanted_ref[owner * capacity + slot].astype(FLOAT32), names)
        for head in range(heads):
            out_refs[head][0, pl.ds(slot * QBLOCK, QBLOCK), :] = held[
                block, :, pl.ds(head * XHEAD, XHEAD)
            ]
    for head in range(heads):
        out_refs[head][0, pl.ds(capacity * QBLOCK, extra), :] = names.astype(BFLOAT)


def pack_queries(asking, wanted, dots, score_gain, payload, capacity):
    rows, width = dots.shape
    heads = width // XHEAD
    owners = payload[0]
    return pl.pallas_call(
        functools.partial(pack_kernel, capacity),
        grid_spec=pltpu.PrefetchScalarGridSpec(
            num_scalar_prefetch=2,
            grid=(owners,),
            in_specs=[
                pl.BlockSpec((rows, width), lambda i, *_: (0, 0)),
                pl.BlockSpec((1, width), lambda i, *_: (0, 0)),
            ],
            out_specs=[pl.BlockSpec((1,) + payload[1:], lambda i, *_: (i, 0, 0))] * heads,
            scratch_shapes=[pltpu.VMEM((rows // QBLOCK, QBLOCK, width), BFLOAT)],
        ),
        out_shape=[jax.ShapeDtypeStruct(payload, BFLOAT)] * heads,
        compiler_params=pltpu.CompilerParams(dimension_semantics=("arbitrary",)),
        cost_estimate=pl.CostEstimate(
            flops=rows * width * 8, bytes_accessed=rows * width * 12, transcendentals=0
        ),
    )(asking, wanted, dots, score_gain.reshape(1, width))


def partial_kernel(capacity, ids_ref, query_ref, key_ref, value_ref, out_ref):
    base = pl.program_id(0) * capacity
    length = key_ref.shape[1]
    ones = jnp.ones((8, length), BFLOAT)
    extra = out_ref.shape[1] - capacity * QBLOCK
    row = lax.broadcasted_iota(jnp.int32, (extra, XHEAD), 0)
    totals = jnp.zeros((extra, XHEAD), FLOAT32)
    for slot in range(capacity):
        passage = ids_ref[base + slot]
        span = pl.ds(slot * QBLOCK, QBLOCK)
        scores = raw_dot(query_ref[0, span, :], key_ref[passage], ((1,), (1,))) * XHEAD ** (-0.5)
        expon = jnp.exp(scores).astype(BFLOAT)
        out_ref[0, span, :] = raw_dot(expon, value_ref[passage], ((1,), (0,))).astype(BFLOAT)
        sums = raw_dot(ones, expon, ((1,), (1,)))[:1]
        high = sums.astype(BFLOAT).astype(FLOAT32)
        middle = (sums - high).astype(BFLOAT).astype(FLOAT32)
        low = sums - high - middle
        line = jnp.concatenate(
            [high, middle, low] + [jnp.zeros_like(low)] * (XHEAD // QBLOCK - 3), axis=1
        )
        totals = jnp.where(row == slot, line, totals)
    out_ref[0, pl.ds(capacity * QBLOCK, extra), :] = totals.astype(BFLOAT)


def partial_attention(ids, queries, keys, values, capacity, head):
    owners, rows, _ = queries.shape
    whole = pl.BlockSpec(keys.shape[:2] + (XHEAD,), lambda i, ids: (0, 0, head))
    piece = pl.BlockSpec((1, rows, XHEAD), lambda i, ids: (i, 0, 0))
    return pl.pallas_call(
        functools.partial(partial_kernel, capacity),
        grid_spec=pltpu.PrefetchScalarGridSpec(
            num_scalar_prefetch=1,
            grid=(owners,),
            in_specs=[piece, whole, whole],
            out_specs=piece,
        ),
        out_shape=jax.ShapeDtypeStruct(queries.shape, BFLOAT),
        compiler_params=pltpu.CompilerParams(
            dimension_semantics=("arbitrary",), vmem_limit_bytes=32 * 1024 * 1024
        ),
        cost_estimate=pl.CostEstimate(
            flops=owners * rows * XHEAD * keys.shape[1] * 8,
            bytes_accessed=owners * rows * XHEAD * 4,
            transcendentals=0,
        ),
    )(ids, queries, keys, values)


def combine_kernel(per_block, capacity, owner_ref, rank_ref, parts_ref, out_ref):
    blocks = out_ref.shape[0] // QBLOCK
    extra = parts_ref.shape[1] - capacity * QBLOCK
    row = lax.broadcasted_iota(jnp.int32, (extra, XHEAD), 0)
    diagonal = lax.broadcasted_iota(jnp.int32, (QBLOCK, QBLOCK), 0) == lax.broadcasted_iota(
        jnp.int32, (QBLOCK, QBLOCK), 1
    )
    for block in range(blocks):
        total = jnp.zeros((QBLOCK, XHEAD), FLOAT32)
        lines = jnp.zeros((extra, XHEAD), FLOAT32)
        for place in range(per_block):
            owner = owner_ref[block * per_block + place]
            rank = rank_ref[block * per_block + place]
            start = pl.multiple_of(rank * QBLOCK, QBLOCK)
            total = total + parts_ref[owner, pl.ds(start, QBLOCK), :].astype(FLOAT32)
            tail = parts_ref[owner, pl.ds(capacity * QBLOCK, extra), :].astype(FLOAT32)
            lines = lines + jnp.where(row == rank, tail, 0.0)
        line = jnp.sum(lines, axis=0, keepdims=True)
        sums = (
            line[:, :QBLOCK] + line[:, QBLOCK : 2 * QBLOCK] + line[:, 2 * QBLOCK : 3 * QBLOCK]
        )
        column = jnp.sum(jnp.where(diagonal, 1.0 / sums, 0.0), axis=1, keepdims=True)
        out_ref[pl.ds(block * QBLOCK, QBLOCK), :] = (total * column).astype(BFLOAT)


def combine(owner_of, slot_rank, parts, capacity, block_count):
    per_block = owner_of.shape[0] // block_count
    return pl.pallas_call(
        functools.partial(combine_kernel, per_block, capacity),
        grid_spec=pltpu.PrefetchScalarGridSpec(
            num_scalar_prefetch=2,
            grid=(1,),
            in_specs=[pl.BlockSpec(parts.shape, lambda i, *_: (0, 0, 0))],
            out_specs=pl.BlockSpec((block_count * QBLOCK, XHEAD), lambda i, *_: (0, 0)),
        ),
        out_shape=jax.ShapeDtypeStruct((block_count * QBLOCK, XHEAD), BFLOAT),
        compiler_params=pltpu.CompilerParams(dimension_semantics=("arbitrary",)),
        cost_estimate=pl.CostEstimate(
            flops=parts.size * 4, bytes_accessed=parts.size * 3, transcendentals=0
        ),
    )(owner_of, slot_rank, parts)


def spread_product(piece, weights):
    count = lax.axis_size("tp")
    me = lax.axis_index("tp")
    total = None
    for shift in range(count):
        moved = piece
        if shift:
            moved = lax.ppermute(piece, "tp", [(i, (i ^ shift)) for i in range(count)])
        rows = lax.dynamic_index_in_dim(weights, me ^ shift, 0, keepdims=False)
        term = jnp.dot(moved, rows, preferred_element_type=FLOAT32)
        total = term if total is None else total + term
    return total


def mixer(
    tokens,
    mix_query,
    mix_key,
    mix_value,
    decay_lower_map,
    decay_upper_map,
    decay_base,
    decay_shift,
    rate_lower_map,
    rate_upper_map,
    norm_gain,
):
    head_count = decay_shift.shape[1]
    head_size = mix_query.shape[1] // head_count

    def project(weight):
        return jnp.dot(tokens, weight, preferred_element_type=FLOAT32).astype(BFLOAT)

    query_vec = project(mix_query)
    key_vec = project(mix_key)
    value_vec = project(mix_value)
    decay_low = jnp.tanh(
        jnp.dot(tokens, decay_lower_map, preferred_element_type=FLOAT32)
    ).astype(BFLOAT)
    decay_pre = (
        decay_base
        + jnp.dot(decay_low, decay_upper_map, preferred_element_type=FLOAT32)
        + jnp.repeat(decay_shift, head_size, axis=1)
    )
    log_fade = -jnp.exp(-jax.nn.softplus(-decay_pre) - 0.5)
    rate_low = jnp.dot(tokens, rate_lower_map, preferred_element_type=FLOAT32).astype(BFLOAT)
    rate_gate = jax.nn.sigmoid(jnp.dot(rate_low, rate_upper_map, preferred_element_type=FLOAT32))
    return recurrence(
        head_count, query_vec, key_vec, value_vec, log_fade, rate_gate, norm_gain
    )


def layer(
    tokens,
    mix_query,
    mix_key,
    mix_value,
    decay_lower_map,
    decay_upper_map,
    decay_base,
    decay_shift,
    rate_lower_map,
    rate_upper_map,
    norm_gain,
    mix_out,
    cross_query,
    score_gain,
    passage_key,
    passage_value,
    cross_out,
    gate_down,
    gate_up,
    store,
    passage_ids,
):
    model_width = tokens.shape[1]
    owner_count = lax.axis_size("st")
    pass_dev = store.shape[0]
    passage_len = store.shape[1]
    cross_width = cross_query.shape[1]
    head_count = cross_width // XHEAD
    block_count, per_block = passage_ids.shape
    flat_ids = passage_ids.reshape(-1)
    slot_count = flat_ids.shape[0]
    capacity = max(2, -(-slot_count // owner_count))
    owner_of = flat_ids // pass_dev
    local_idx = flat_ids % pass_dev
    slot_order = jnp.arange(slot_count)
    earlier_same = (owner_of[:, None] == owner_of[None, :]) & (
        slot_order[None, :] < slot_order[:, None]
    )
    slot_rank = jnp.sum(earlier_same.astype(jnp.int32), axis=1)
    to_owner = owner_of[:, None] == jnp.arange(owner_count)[None, :]
    to_slot = slot_rank[:, None] == jnp.arange(capacity)[None, :]
    chosen = to_owner[:, :, None] & to_slot[:, None, :]
    wanted = jnp.sum(jnp.where(chosen, local_idx[:, None, None], 0), axis=0)
    asking = jnp.sum(jnp.where(chosen, (slot_order // per_block)[:, None, None], 0), axis=0)

    extra = -(-capacity // 8) * 8
    payload = (owner_count, capacity * QBLOCK + extra, XHEAD)

    def exchange(values):
        return lax.all_to_all(values, "st", split_axis=0, concat_axis=0, tiled=True)

    dots = jnp.dot(tokens, cross_query, preferred_element_type=FLOAT32)
    outgoing = pack_queries(
        asking.reshape(-1), wanted.reshape(-1), dots, score_gain, payload, capacity
    )
    incoming = [exchange(outgoing[head]) for head in range(head_count)]
    flat_rows = store.reshape(-1, model_width)
    keyed = head_norm(
        jnp.dot(flat_rows, passage_key, preferred_element_type=FLOAT32), XHEAD
    ).astype(BFLOAT)
    valued = jnp.dot(flat_rows, passage_value, preferred_element_type=FLOAT32).astype(BFLOAT)
    keyed = keyed.reshape(pass_dev, passage_len, cross_width)
    valued = valued.reshape(pass_dev, passage_len, cross_width)
    parts = []
    for head in range(head_count):
        if head == 0:
            names = incoming[0][:, capacity * QBLOCK : capacity * QBLOCK + capacity, 0]
            served = names.astype(jnp.int32).reshape(-1)
        part = partial_attention(served, incoming[head], keyed, valued, capacity, head)
        parts.append(exchange(part))
    mixer_heads = mixer(
        tokens,
        mix_query,
        mix_key,
        mix_value,
        decay_lower_map,
        decay_upper_map,
        decay_base,
        decay_shift,
        rate_lower_map,
        rate_upper_map,
        norm_gain,
    )
    shard_total = lax.axis_size("tp")
    out_cols = mix_out.shape[1]
    mixer_part = lax.optimization_barrier(
        spread_product(mixer_heads, mix_out.reshape(shard_total, -1, out_cols))
    )
    gate_low = jnp.dot(tokens, gate_down, preferred_element_type=FLOAT32).astype(BFLOAT)
    gate_open = lax.optimization_barrier(
        jax.nn.sigmoid(jnp.dot(gate_low, gate_up, preferred_element_type=FLOAT32))
    )
    cross_rows = cross_out.reshape(shard_total, head_count, XHEAD, out_cols)
    cross_part = None
    for head in range(head_count):
        attended = combine(owner_of, slot_rank, parts[head], capacity, block_count)
        term = spread_product(attended, cross_rows[:, head])
        if head < head_count - 1:
            term = lax.optimization_barrier(term)
        cross_part = term if cross_part is None else cross_part + term
    return (mixer_part + gate_open * cross_part).astype(BFLOAT)


def solution(mesh):
    placed = (
        P("st", None),
        P(None, "tp"),
        P(None, "tp"),
        P(None, "tp"),
        P(),
        P(None, "tp"),
        P("tp"),
        P("st", "tp"),
        P(),
        P(None, "tp"),
        P("tp"),
        P(None, "tp"),
        P(None, "tp"),
        P("tp"),
        P(None, "tp"),
        P(None, "tp"),
        P(None, "tp"),
        P(),
        P(None, "tp"),
        P("st", None, None),
        P("st", None),
    )
    return jax.shard_map(
        layer, mesh=mesh, in_specs=placed, out_specs=P("st", "tp"), check_vma=False
    )
```
